32 devices in a mesh: sp: 8 (over z, y), tp: 4 (over x, core).
Axes of the slice: x: 2, y: 2, z: 4, core: 2. Of those that a mesh axis runs over, the one named last changes fastest.
Arguments:
- latent: bfloat16 [3072, 2048], P(('sp', 'tp')), may hold values from -6 to 6
- context: bfloat16 [512, 2048], P('sp'), may hold values from -6 to 6
- cond_latent: float32 [2048], replicated, may hold values from -6 to 6
- cond_context: float32 [2048], replicated, may hold values from -12 to 12
- shift_weight: bfloat16 [2048, 2048], P('sp', 'tp'), may hold values from -0.125 to 0.125
- scale_weight: bfloat16 [2048, 2048], P('sp', 'tp'), may hold values from -0.125 to 0.125
- gate_weight: bfloat16 [2048, 2048], P('sp', 'tp'), may hold values from -0.125 to 0.125
- query_weight: bfloat16 [2, 2048, 1024], P(None, None, 'tp'), may hold values from -1.3258252 to 1.3258252
- key_weight: bfloat16 [2, 2048, 1024], P(None, None, 'tp'), may hold values from -1.3258252 to 1.3258252
- value_weight: bfloat16 [2048, 2048], P(None, 'tp'), may hold values from -0.125 to 0.125
- out_weight: bfloat16 [2048, 2048], P('tp'), may hold values from -0.125 to 0.125
- lambda_heads: float32 [16], P('tp'), may hold values from 0.3 to 0.8
- out_gain: float32 [2048], P('tp'), may hold values from 0.1 to 1.9
Outputs:
- result: bfloat16 [3072, 2048], P(('sp', 'tp'))
The draws below stay inside these ranges and needn't reach their ends.
All inputs are finite; a program needn't handle non-finite values.
Results may differ from the reference program's by a relative error of at most 0.02.
The reference program's roundings to bfloat16 on the way count: a program that leaves them out, or rounds other values in their place, can miss the bound.
Values may be sent and summed in bfloat16 or wider, within the bound.
A program may use at most 128 MiB of HBM per device.

```python
import math
import jax
import jax.numpy as jnp
from jax import lax

D = 2048
HEADS = 16
HEAD_DIM = 64
GRID_W = 64
CTX = 512
VALUE_DIM = 128
TOKENS = 3072
N_TP = 4


def projection(key, salt_value):
    entries = jax.random.truncated_normal(jax.random.fold_in(key, salt_value), -6.0, 6.0, (2, D, HEADS, HEAD_DIM), jnp.float32)
    scaled = entries * D ** (-0.5)
    return scaled.reshape(2, D, HEADS * HEAD_DIM).astype(jnp.bfloat16)


def draw_query_weight(key, part):
    return projection(key, 11)


def draw_key_weight(key, part):
    return projection(key, 23)


def level_of(own_key, extent, shards, low, top_value):
    gain = 1.0
    for dim, shards_of in shards:
        steps = jax.random.uniform(jax.random.fold_in(jax.random.fold_in(own_key, 6), dim), (shards_of,), jnp.float32, low / len(shards), top_value / len(shards))
        gain = gain * jnp.repeat(jnp.exp(steps), extent[dim] // shards_of).reshape((-1,) + (1,) * (len(extent) - 1 - dim))
    return gain


def gaussian(stream_key, extent, spread, reach, cuts=(), held_as=jnp.bfloat16):
    values = spread * jax.random.normal(stream_key, extent, jnp.float32)
    if cuts:
        values = values * level_of(stream_key, extent, cuts, -0.22, 0.18)
    return jnp.clip(values, -reach, reach).astype(held_as)


def setup_inputs(seed: int = 0) -> dict:
    streams_of = jax.random.split(jax.random.key(seed), 14)
    latent = gaussian(streams_of[0], (TOKENS, D), 1.0, 6.0, ((0, 32),))
    context = gaussian(streams_of[1], (CTX, D), 1.0, 6.0, ((0, 8),))
    cond_latent = gaussian(streams_of[2], (D,), 1.0, 6.0, (), jnp.float32)
    cond_context = gaussian(streams_of[3], (D,), 2.0, 12.0, (), jnp.float32)
    shift_weight = gaussian(streams_of[4], (D, D), D ** -0.5, 0.125, ((0, 8), (1, 4)))
    scale_weight = gaussian(streams_of[5], (D, D), D ** -0.5, 0.125, ((0, 8), (1, 4)))
    gate_weight = gaussian(streams_of[6], (D, D), D ** -0.5, 0.125, ((0, 8), (1, 4)))
    query_weight = draw_query_weight(jax.random.fold_in(streams_of[13], 71), 0)
    key_weight = draw_key_weight(jax.random.fold_in(streams_of[13], 71), 0)
    value_weight = gaussian(streams_of[9], (D, HEADS * VALUE_DIM), D ** -0.5, 0.125, ((1, 4),))
    out_weight = gaussian(streams_of[10], (HEADS * VALUE_DIM, D), (HEADS * VALUE_DIM) ** -0.5, 0.125, ((0, 4),))
    lambda_heads = jnp.clip(0.3 + 0.5 * jax.random.uniform(streams_of[11], (HEADS,), jnp.float32) ** level_of(streams_of[11], (HEADS,), ((0, 4),), -0.2, 0.2), 0.3, 0.8)
    out_gain = jnp.clip(1.0 + 0.18 * jax.random.normal(streams_of[12], (HEADS * VALUE_DIM,), jnp.float32), 0.1, 1.9)
    return dict(latent=latent, context=context, cond_latent=cond_latent, cond_context=cond_context, shift_weight=shift_weight, scale_weight=scale_weight, gate_weight=gate_weight, query_weight=query_weight, key_weight=key_weight, value_weight=value_weight, out_weight=out_weight, lambda_heads=lambda_heads, out_gain=out_gain)


norm_eps = 1e-06
rope_theta = 10000.0

def rms_scale(matrix):
    return matrix * lax.rsqrt(lax.optimization_barrier(jnp.mean(matrix * matrix, axis=-1, keepdims=True)) + norm_eps)

def modulated(activations, shift, scale):
    return (rms_scale(activations.astype(jnp.float32)) * (1.0 + scale) + shift).astype(jnp.bfloat16)

def rotate(vectors, positions, grid_width):
    quarter = vectors.shape[-1] // 4
    inverse = rope_theta ** (-jnp.arange(quarter, dtype=jnp.float32) / quarter)
    grid_row = (positions // grid_width).astype(jnp.float32)
    grid_col = (positions % grid_width).astype(jnp.float32)
    angles = jnp.concatenate([grid_row[:, None] * inverse, grid_col[:, None] * inverse], axis=-1)
    cos_table = jnp.cos(angles)[:, None, :]
    sin_table = jnp.sin(angles)[:, None, :]
    former = vectors[..., :2 * quarter]
    latter = vectors[..., 2 * quarter:]
    return jnp.concatenate([former * cos_table - latter * sin_table, latter * cos_table + former * sin_table], axis=-1)

def reference(latent, context, cond_latent, cond_context, shift_weight, scale_weight, gate_weight, query_weight, key_weight, value_weight, out_weight, lambda_heads, out_gain):
    conditions = jax.nn.silu(jnp.stack([cond_latent, cond_context])).astype(jnp.bfloat16)
    shifts = jnp.dot(conditions, shift_weight, preferred_element_type=jnp.float32)
    scales = jnp.dot(conditions, scale_weight, preferred_element_type=jnp.float32)
    gate_vector = jnp.dot(conditions[:1], gate_weight, preferred_element_type=jnp.float32)[0]
    hidden = modulated(latent, shifts[0], scales[0])
    context_hidden = modulated(context, shifts[1], scales[1])
    positions = jnp.arange(TOKENS, dtype=jnp.int32)

    def latent_heads(weight):
        product = jnp.dot(hidden, weight, preferred_element_type=jnp.float32).reshape(TOKENS, HEADS, HEAD_DIM)
        return rotate(product, positions, GRID_W).astype(jnp.bfloat16)

    def context_heads(weight):
        product = jnp.dot(context_hidden, weight, preferred_element_type=jnp.float32)
        return product.reshape(CTX, HEADS, HEAD_DIM).astype(jnp.bfloat16)
    queries = jnp.stack([latent_heads(query_weight[0]), latent_heads(query_weight[1])])
    key_rows = jnp.stack([jnp.concatenate([context_heads(key_weight[which_map]), latent_heads(key_weight[which_map])], axis=0) for which_map in (0, 1)])
    value_rows = jnp.concatenate([jnp.dot(context_hidden, value_weight, preferred_element_type=jnp.float32).astype(jnp.bfloat16), jnp.dot(hidden, value_weight, preferred_element_type=jnp.float32).astype(jnp.bfloat16)], axis=0)
    queries, key_rows, value_rows = lax.optimization_barrier((queries, key_rows, value_rows))
    queries = queries.transpose(2, 0, 1, 3)
    key_rows = key_rows.transpose(2, 0, 1, 3)
    value_rows = value_rows.reshape(CTX + TOKENS, HEADS, VALUE_DIM).transpose(1, 0, 2)
    query_block = math.gcd(TOKENS, 512)

    def one_head(operands):
        head_queries, head_keys, head_values, head_lambda = operands
        key_float = head_keys.astype(jnp.float32)
        value_float = head_values.astype(jnp.float32)
        blocks = head_queries.reshape(2, TOKENS // query_block, query_block, HEAD_DIM).transpose(1, 0, 2, 3)

        def one_block(block_queries):
            scores = jnp.einsum('mqd,mkd->mqk', block_queries.astype(jnp.float32), key_float) * HEAD_DIM ** (-0.5)
            weights = jnp.exp(scores - lax.optimization_barrier(jnp.max(scores, axis=-1, keepdims=True)))
            totals = lax.optimization_barrier(jnp.sum(weights, axis=-1, keepdims=True))
            rounded = lax.optimization_barrier(weights.astype(jnp.bfloat16)).astype(jnp.float32)
            numerator = jnp.einsum('mqk,ke->mqe', rounded, value_float)
            return numerator[0] / totals[0] - head_lambda * (numerator[1] / totals[1])
        return lax.map(one_block, blocks).reshape(TOKENS, VALUE_DIM)
    mixed = lax.map(one_head, (queries, key_rows, value_rows, lambda_heads))
    normed = rms_scale(mixed) * out_gain.reshape(HEADS, 1, VALUE_DIM)
    heads_out = normed.transpose(1, 0, 2).reshape(TOKENS, HEADS * VALUE_DIM).astype(jnp.bfloat16)
    group_width = HEADS // N_TP * VALUE_DIM
    summed = jnp.zeros((TOKENS, D), jnp.float32)
    for group_index in range(N_TP):
        lower = group_index * group_width
        group_term = jnp.dot(heads_out[:, lower:lower + group_width], out_weight[lower:lower + group_width], preferred_element_type=jnp.float32)
        summed = summed + lax.optimization_barrier(group_term.astype(jnp.bfloat16)).astype(jnp.float32)
    return (latent.astype(jnp.float32) + gate_vector * summed).astype(jnp.bfloat16)
```

```python
import functools

import jax
import jax.numpy as jnp
from jax import lax
from jax.experimental import pallas as pl
from jax.experimental.pallas import tpu as pltpu
from jax.sharding import PartitionSpec as P

HEAD_DIM = 64
GRID_W = 64
VALUE_DIM = 128
LANES = 128

norm_eps = 1e-06
rope_theta = 10000.0
f32 = jnp.float32
bf16 = jnp.bfloat16
MESH = pl.DeviceIdType.MESH


def pick(total, limit, unit):
    best = unit
    for size in range(unit, limit + 1, unit):
        if total % size == 0:
            best = size
    return best


def body(
    n_sp,
    n_tp,
    lat,
    ctx,
    cond_l,
    cond_c,
    shift_w,
    scale_w,
    gate_w,
    lane_table,
    lam,
    gain,
    wq_hbm,
    wk_hbm,
    wv_hbm,
    wo_hbm,
    out,
    wq,
    wk,
    wv,
    wo,
    mod_part,
    mod_recv,
    mod_all,
    raw,
    hidden,
    cos_t,
    sin_t,
    q_send,
    kv_send,
    kvc_send,
    q_buf,
    kv_buf,
    scores,
    o_send,
    heads,
    pair_send,
    pair_recv,
    fin_send,
    fin_recv,
    own_sum,
    w_sem,
    loc_sem,
    mod1_s,
    mod1_r,
    mod2_s,
    mod2_r,
    raw_s,
    raw_r,
    fwd_s,
    fwd_r,
    q_s,
    q_r,
    kv_s,
    kv_r,
    kvc_s,
    kvc_r,
    rel_s,
    rel_r,
    relc_s,
    relc_r,
    o_s,
    o_r,
    pair_s,
    pair_r,
    fin_s,
    fin_r,
):
    own, width = lat.shape
    ctx_rows = ctx.shape[0]
    tok = own * n_tp
    mod_cols = shift_w.shape[1]
    groups = q_send.shape[0]
    ranks = n_sp // groups
    chips = n_tp // 2
    sp_i = lax.axis_index("sp")
    tp_i = lax.axis_index("tp")
    g_i = sp_i // ranks
    r_i = sp_i % ranks
    chip_i = tp_i // 2
    core_i = tp_i % 2
    partner = chip_i * 2 + (1 - core_i)
    pending = []

    def send(src, dst, s_sem, r_sem, **where):
        copy = pltpu.make_async_remote_copy(
            src_ref=src, dst_ref=dst, send_sem=s_sem, recv_sem=r_sem,
            device_id=where, device_id_type=MESH,
        )
        copy.start()
        pending.append(copy)

    def arrived(ref, s_sem, r_sem, **where):
        pltpu.make_async_remote_copy(
            src_ref=ref, dst_ref=ref, send_sem=s_sem, recv_sem=r_sem,
            device_id=where, device_id_type=MESH,
        ).wait_recv()

    loads = [
        pltpu.make_async_copy(src, dst, w_sem.at[i])
        for i, (src, dst) in enumerate(
            ((wk_hbm, wk), (wv_hbm, wv), (wq_hbm, wq), (wo_hbm, wo))
        )
    ]
    for load in loads:
        load.start()

    barrier = pltpu.get_barrier_semaphore()
    for k in range(1, n_sp):
        pl.semaphore_signal(
            barrier, inc=1, device_id={"sp": (sp_i + k) % n_sp}, device_id_type=MESH
        )
    for k in range(1, n_tp):
        pl.semaphore_signal(
            barrier, inc=1, device_id={"tp": (tp_i + k) % n_tp}, device_id_type=MESH
        )

    def silu(v):
        return (v / (1.0 + jnp.exp(-v))).astype(bf16).astype(f32)

    c0 = silu(cond_l[sp_i])
    c1 = silu(cond_c[sp_i])
    row = lax.broadcasted_iota(jnp.int32, (8, c0.shape[-1]), 0)

    def placed_rows(at0, at1):
        zero = jnp.zeros(row.shape, f32)
        rows = jnp.where(row == at0, jnp.broadcast_to(c0, row.shape), zero)
        if at1 is not None:
            rows = jnp.where(row == at1, jnp.broadcast_to(c1, row.shape), rows)
        return rows.astype(bf16)

    mod_part[...] = (
        jnp.dot(placed_rows(0, 1), shift_w[...], preferred_element_type=f32)
        + jnp.dot(placed_rows(2, 3), scale_w[...], preferred_element_type=f32)
        + jnp.dot(placed_rows(4, None), gate_w[...], preferred_element_type=f32)
    )
    pl.semaphore_wait(barrier, n_sp + n_tp - 2)

    for k in range(1, n_sp):
        send(
            mod_part, mod_recv.at[sp_i], mod1_s.at[k], mod1_r.at[sp_i], sp=(sp_i + k) % n_sp
        )
    for k in range(1, chips):
        send(
            lat, raw.at[tp_i], raw_s.at[k], raw_r.at[chip_i],
            tp=((chip_i + k) % chips) * 2 + core_i,
        )
    send(lat, raw.at[tp_i], fwd_s.at[0], fwd_r.at[chip_i], tp=partner)
    raw[tp_i] = lat[...]
    mod_recv[sp_i] = mod_part[...]

    tok_row = lax.broadcasted_iota(jnp.int32, (tok, LANES), 0) + sp_i * tok
    grid_row = (tok_row // GRID_W).astype(f32)
    grid_col = (tok_row % GRID_W).astype(f32)
    angles = grid_row * lane_table[0:1, :] + grid_col * lane_table[1:2, :]
    cos_t[...] = jnp.cos(angles)
    sin_t[...] = jnp.sin(angles) * lane_table[2:3, :]

    for k in range(1, n_sp):
        src = (sp_i + n_sp - k) % n_sp
        arrived(mod_recv.at[src], mod1_s.at[k], mod1_r.at[src], sp=src)
    total = mod_recv[0]
    for s in range(1, n_sp):
        total = total + mod_recv[s]
    mod_part2 = mod_all.at[tp_i]
    mod_part2[...] = total
    for k in range(1, n_tp):
        send(
            mod_part2, mod_all.at[tp_i], mod2_s.at[k], mod2_r.at[tp_i], tp=(tp_i + k) % n_tp
        )
    for k in range(1, chips):
        src_chip = (chip_i + chips - k) % chips
        slot = src_chip * 2 + core_i
        arrived(raw.at[slot], raw_s.at[k], raw_r.at[src_chip], tp=slot)
        send(raw.at[slot], raw.at[slot], fwd_s.at[k], fwd_r.at[src_chip], tp=partner)
    for k in range(1, n_tp):
        src = (tp_i + n_tp - k) % n_tp
        arrived(mod_all.at[src], mod2_s.at[k], mod2_r.at[src], tp=src)

    def modulate(x, which, start):
        rows = x.shape[0]
        factor = lax.rsqrt(jnp.mean(x * x, axis=-1, keepdims=True) + norm_eps)
        for t in range(n_tp):
            cols = slice(t * mod_cols, (t + 1) * mod_cols)
            shift = mod_all[t, which : which + 1, :]
            scale = mod_all[t, which + 2 : which + 3, :]
            hidden[start : start + rows, cols] = (
                (x[:, cols] * factor) * (1.0 + scale) + shift
            ).astype(bf16)

    modulate(ctx[...].astype(f32), 1, tok)
    for k in range(chips):
        src_chip = (chip_i + chips - k) % chips
        slot = src_chip * 2 + (1 - core_i)
        arrived(raw.at[slot], fwd_s.at[k], fwd_r.at[src_chip], tp=partner)
    for t in range(n_tp):
        modulate(raw[t].astype(f32), 0, t * own)

    lane = lax.broadcasted_iota(jnp.int32, (tok, LANES), 1)
    first_quarter = lane % HEAD_DIM < HEAD_DIM // 2
    ctx_half = lax.broadcasted_iota(jnp.int32, (ctx_rows, LANES), 1) < HEAD_DIM

    def rope(u):
        swapped = jnp.where(
            first_quarter,
            pltpu.roll(u, LANES - HEAD_DIM // 2, 1),
            pltpu.roll(u, HEAD_DIM // 2, 1),
        )
        return u * cos_t[...] + swapped * sin_t[...]

    def pair_up(a, b, low):
        return (
            jnp.where(low, a, pltpu.roll(b, HEAD_DIM, 1)).astype(bf16),
            jnp.where(low, pltpu.roll(a, HEAD_DIM, 1), b).astype(bf16),
        )

    low_half = lane < HEAD_DIM
    loads[0].wait()
    keys = [jnp.dot(hidden[...], wk[m], preferred_element_type=f32) for m in (0, 1)]
    for p in range(groups // 2):
        slab = slice(p * LANES, (p + 1) * LANES)
        a, b = pair_up(rope(keys[0][:tok, slab]), rope(keys[1][:tok, slab]), low_half)
        kv_send[2 * p, :, :LANES] = a
        kv_send[2 * p + 1, :, :LANES] = b
        a, b = pair_up(keys[0][tok:, slab], keys[1][tok:, slab], ctx_half)
        kvc_send[2 * p, :, :LANES] = a
        kvc_send[2 * p + 1, :, :LANES] = b
    loads[1].wait()
    vals = jnp.dot(hidden[...], wv[...], preferred_element_type=f32).astype(bf16)
    for j in range(groups):
        slab = slice(j * LANES, (j + 1) * LANES)
        kv_send[j, :, LANES:] = vals[:tok, slab]
        kvc_send[j, :, LANES:] = vals[tok:, slab]

    def lat_slot(s):
        return kv_buf.at[pl.ds(pl.multiple_of(s * tok, 16), tok)]

    def ctx_slot(s):
        return kv_buf.at[pl.ds(pl.multiple_of(n_sp * tok + s * ctx_rows, 16), ctx_rows)]

    order = list(range(1, groups))
    for k in order:
        g = (g_i + k) % groups
        send(kv_send.at[g], lat_slot(sp_i), kv_s.at[k], kv_r.at[g_i], sp=g * ranks + r_i)
        send(kvc_send.at[g], ctx_slot(sp_i), kvc_s.at[k], kvc_r.at[g_i], sp=g * ranks + r_i)
    for e in range(1, ranks):
        to = g_i * ranks + (r_i + e) % ranks
        send(kv_send.at[g_i], lat_slot(sp_i), rel_s.at[0, e], rel_r.at[g_i, r_i], sp=to)
        send(kvc_send.at[g_i], ctx_slot(sp_i), relc_s.at[0, e], relc_r.at[g_i, r_i], sp=to)
    local = [
        pltpu.make_async_copy(kv_send.at[g_i], lat_slot(sp_i), loc_sem.at[0]),
        pltpu.make_async_copy(kvc_send.at[g_i], ctx_slot(sp_i), loc_sem.at[1]),
    ]
    for copy in local:
        copy.start()

    loads[2].wait()
    queries = [jnp.dot(hidden[:tok, :], wq[m], preferred_element_type=f32) for m in (0, 1)]
    for p in range(groups // 2):
        slab = slice(p * LANES, (p + 1) * LANES)
        a, b = pair_up(rope(queries[0][:, slab]), rope(queries[1][:, slab]), low_half)
        q_send[2 * p] = a
        q_send[2 * p + 1] = b
    for k in order:
        g = (g_i + k) % groups
        send(q_send.at[g], q_buf.at[g_i], q_s.at[k], q_r.at[g_i], sp=g * ranks + r_i)
    q_local = pltpu.make_async_copy(q_send.at[g_i], q_buf.at[g_i], loc_sem.at[2])
    q_local.start()

    for k in order:
        g = (g_i + groups - k) % groups
        s = g * ranks + r_i
        arrived(lat_slot(s), kv_s.at[k], kv_r.at[g], sp=s)
        for e in range(1, ranks):
            to = g_i * ranks + (r_i + e) % ranks
            send(lat_slot(s), lat_slot(s), rel_s.at[k, e], rel_r.at[g, r_i], sp=to)
        arrived(ctx_slot(s), kvc_s.at[k], kvc_r.at[g], sp=s)
        for e in range(1, ranks):
            to = g_i * ranks + (r_i + e) % ranks
            send(ctx_slot(s), ctx_slot(s), relc_s.at[k, e], relc_r.at[g, r_i], sp=to)
    for copy in local:
        copy.wait()
    q_local.wait()
    for k in order:
        g = (g_i + groups - k) % groups
        arrived(q_buf.at[g], q_s.at[k], q_r.at[g], sp=g * ranks + r_i)
    for e in range(1, ranks):
        r = (r_i + ranks - e) % ranks
        for k in range(groups):
            g = (g_i + groups - k) % groups
            s = g * ranks + r
            arrived(lat_slot(s), rel_s.at[k, e], rel_r.at[g, r], sp=g_i * ranks + r)
            arrived(ctx_slot(s), relc_s.at[k, e], relc_r.at[g, r], sp=g_i * ranks + r)

    key_total = kv_buf.shape[0]
    q_tile = scores.shape[0] // 2
    block = pick(key_total, 512, LANES)
    coef = HEAD_DIM ** (-0.5) * 1.4426950408889634
    q_low = lax.broadcasted_iota(jnp.int32, (q_tile, LANES), 1) < HEAD_DIM
    head_lam = lam[g_i]
    head_gain = gain[g_i]

    def attend(g, start):
        q = q_buf[g, pl.ds(start, q_tile), :]
        zero = jnp.zeros_like(q)
        q2 = jnp.concatenate([jnp.where(q_low, q, zero), jnp.where(q_low, zero, q)], axis=0)
        peak = None
        for b in range(key_total // block):
            rows = slice(b * block, (b + 1) * block)
            s = lax.dot_general(
                q2, kv_buf[rows, :LANES], (((1,), (1,)), ((), ())), preferred_element_type=f32
            )
            scores[:, rows] = s
            for c in range(block // LANES):
                piece = s[:, c * LANES : (c + 1) * LANES]
                peak = piece if peak is None else jnp.maximum(peak, piece)
        top = jnp.max(peak, axis=-1, keepdims=True) * coef
        sums = None
        acc = None
        for b in range(key_total // block):
            rows = slice(b * block, (b + 1) * block)
            w = jnp.exp2(scores[:, rows] * coef - top)
            for c in range(block // LANES):
                piece = w[:, c * LANES : (c + 1) * LANES]
                sums = piece if sums is None else sums + piece
            part = jnp.dot(w.astype(bf16), kv_buf[rows, LANES:], preferred_element_type=f32)
            acc = part if acc is None else acc + part
        mean_v = acc / jnp.sum(sums, axis=-1, keepdims=True)
        mixed = mean_v[:q_tile] - head_lam * mean_v[q_tile:]
        factor = lax.rsqrt(jnp.mean(mixed * mixed, axis=-1, keepdims=True) + norm_eps)
        o_send[g, pl.ds(start, q_tile), :] = (mixed * factor * head_gain).astype(bf16)

    def o_copy(k):
        g = (g_i + 1 + k) % groups
        return pltpu.make_async_remote_copy(
            src_ref=o_send.at[g], dst_ref=heads.at[g_i], send_sem=o_s.at[k],
            recv_sem=o_r.at[g_i], device_id={"sp": g * ranks + r_i}, device_id_type=MESH,
        )

    @pl.loop(0, groups)
    def _(k):
        g = (g_i + 1 + k) % groups

        @pl.loop(0, tok // q_tile)
        def _(i):
            attend(g, pl.multiple_of(i * q_tile, q_tile))

        @pl.when(k < groups - 1)
        def _():
            o_copy(k).start()

    heads[g_i] = o_send[g_i]
    loads[3].wait()
    for k in range(groups - 1):
        src = (g_i + groups - 1 - k) % groups
        arrived(heads.at[src], o_s.at[k], o_r.at[src], sp=src * ranks + r_i)

    def term(chunk):
        start = pl.multiple_of(chunk * own, 16)
        left = jnp.concatenate(
            [heads[h, pl.ds(start, own), :] for h in range(groups)], axis=-1
        )
        return jnp.dot(left, wo[...], preferred_element_type=f32).astype(bf16)

    for k in range(chips):
        chip = (chip_i + 1 + k) % chips
        pair_send[k] = term(chip * 2 + (1 - core_i))
        send(pair_send.at[k], pair_recv.at[k], pair_s.at[k], pair_r.at[k], tp=partner)
    for k in range(chips):
        chip = (chip_i + 1 + k) % chips
        mine = term(chip * 2 + core_i).astype(f32)
        arrived(pair_recv.at[k], pair_s.at[k], pair_r.at[k], tp=partner)
        both = mine + pair_recv[k].astype(f32)
        if k < chips - 1:
            fin_send[k] = both.astype(bf16)
            send(
                fin_send.at[k], fin_recv.at[k], fin_s.at[k], fin_r.at[k], tp=chip * 2 + core_i
            )
        else:
            own_sum[...] = both
    for k in range(chips - 1):
        src_chip = (chip_i + chips - 1 - k) % chips
        arrived(fin_recv.at[k], fin_s.at[k], fin_r.at[k], tp=src_chip * 2 + core_i)
    for t in range(n_tp):
        cols = slice(t * mod_cols, (t + 1) * mod_cols)
        summed = own_sum[:, cols]
        for k in range(chips - 1):
            summed = summed + fin_recv[k, :, cols].astype(f32)
        out[:, cols] = (
            lat[:, cols].astype(f32) + mod_all[t, 4:5, :] * summed
        ).astype(bf16)
    for copy in pending:
        copy.wait_send()
    for k in range(groups - 1):
        o_copy(k).wait_send()


def local(
    n_sp,
    n_tp,
    latent,
    context,
    cond_latent,
    cond_context,
    shift_weight,
    scale_weight,
    gate_weight,
    query_weight,
    key_weight,
    value_weight,
    out_weight,
    lambda_heads,
    out_gain,
):
    own, width = latent.shape
    ctx_rows = context.shape[0]
    tok = own * n_tp
    groups = lambda_heads.shape[0]
    ranks = n_sp // groups
    chips = n_tp // 2
    mod_rows, mod_cols = shift_weight.shape
    keys = n_sp * (tok + ctx_rows)
    q_tile = pick(tok, 128, 16)

    quarter = HEAD_DIM // 4
    inverse = rope_theta ** (-jnp.arange(quarter, dtype=f32) / quarter)
    zeros = jnp.zeros((quarter,), f32)
    repeat = LANES // (2 * quarter)
    half = jnp.ones((2 * quarter,), f32)
    lane_table = jnp.stack(
        [
            jnp.tile(jnp.concatenate([inverse, zeros]), repeat),
            jnp.tile(jnp.concatenate([zeros, inverse]), repeat),
            jnp.tile(jnp.concatenate([-half, half]), repeat // 2),
        ]
        + [jnp.zeros((LANES,), f32)] * 5
    )
    lam = jnp.broadcast_to(lambda_heads[:, None, None], (groups, 1, LANES))
    gain = out_gain.reshape(groups, 1, VALUE_DIM)
    vmem = pl.BlockSpec(memory_space=pltpu.VMEM)
    hbm = pl.BlockSpec(memory_space=pl.ANY)
    dma = pltpu.SemaphoreType.DMA
    scratch = [
        pltpu.VMEM(query_weight.shape, bf16),
        pltpu.VMEM(key_weight.shape, bf16),
        pltpu.VMEM(value_weight.shape, bf16),
        pltpu.VMEM(out_weight.shape, bf16),
        pltpu.VMEM((8, mod_cols), f32),
        pltpu.VMEM((n_sp, 8, mod_cols), f32),
        pltpu.VMEM((n_tp, 8, mod_cols), f32),
        pltpu.VMEM((n_tp, own, width), bf16),
        pltpu.VMEM((tok + ctx_rows, width), bf16),
        pltpu.VMEM((tok, LANES), f32),
        pltpu.VMEM((tok, LANES), f32),
        pltpu.VMEM((groups, tok, LANES), bf16),
        pltpu.VMEM((groups, tok, 2 * LANES), bf16),
        pltpu.VMEM((groups, ctx_rows, 2 * LANES), bf16),
        pltpu.VMEM((groups, tok, LANES), bf16),
        pltpu.VMEM((keys, 2 * LANES), bf16),
        pltpu.VMEM((2 * q_tile, keys), f32),
        pltpu.VMEM((groups, tok, LANES), bf16),
        pltpu.VMEM((groups, tok, LANES), bf16),
        pltpu.VMEM((chips, own, width), bf16),
        pltpu.VMEM((chips, own, width), bf16),
        pltpu.VMEM((max(chips - 1, 1), own, width), bf16),
        pltpu.VMEM((max(chips - 1, 1), own, width), bf16),
        pltpu.VMEM((own, width), f32),
        dma((4,)),
        dma((3,)),
        dma((n_sp,)),
        dma((n_sp,)),
        dma((n_tp,)),
        dma((n_tp,)),
        dma((chips,)),
        dma((chips,)),
        dma((chips,)),
        dma((chips,)),
        dma((groups,)),
        dma((groups,)),
        dma((groups,)),
        dma((groups,)),
        dma((groups,)),
        dma((groups,)),
        dma((groups, ranks)),
        dma((groups, ranks)),
        dma((groups, ranks)),
        dma((groups, ranks)),
        dma((groups,)),
        dma((groups,)),
        dma((chips,)),
        dma((chips,)),
        dma((chips,)),
        dma((chips,)),
    ]
    return pl.pallas_call(
        functools.partial(body, n_sp, n_tp),
        out_shape=jax.ShapeDtypeStruct((own, width), bf16),
        in_specs=[vmem] * 10 + [hbm] * 4,
        out_specs=vmem,
        scratch_shapes=scratch,
        compiler_params=pltpu.CompilerParams(
            collective_id=0, has_side_effects=True, vmem_limit_bytes=60 * 1024 * 1024
        ),
        name="diff_attention",
    )(
        latent,
        context,
        cond_latent.reshape(n_sp, 1, mod_rows),
        cond_context.reshape(n_sp, 1, mod_rows),
        shift_weight,
        scale_weight,
        gate_weight,
        lane_table,
        lam,
        gain,
        query_weight,
        key_weight,
        value_weight,
        out_weight,
    )


def solution(mesh):
    placed = (
        P(("sp", "tp"), None),
        P("sp", None),
        P(),
        P(),
        P("sp", "tp"),
        P("sp", "tp"),
        P("sp", "tp"),
        P(None, None, "tp"),
        P(None, None, "tp"),
        P(None, "tp"),
        P("tp", None),
        P("tp"),
        P("tp"),
    )
    return jax.shard_map(
        functools.partial(local, mesh.shape["sp"], mesh.shape["tp"]),
        mesh=mesh,
        in_specs=placed,
        out_specs=P(("sp", "tp"), None),
        check_vma=False,
    )
```

```python
import functools

import jax
import jax.numpy as jnp
import numpy as np
from jax import lax
from jax.experimental import pallas as pl
from jax.experimental.pallas import tpu as pltpu
from jax.sharding import PartitionSpec as P

HEAD_DIM = 64
GRID_W = 64
VALUE_DIM = 128
LANES = 128

norm_eps = 1e-06
rope_theta = 10000.0
f32 = jnp.float32
bf16 = jnp.bfloat16
MESH = pl.DeviceIdType.MESH


def pick(total, limit, unit):
    best = unit
    for size in range(unit, limit + 1, unit):
        if total % size == 0:
            best = size
    return best


def body(
    n_sp,
    n_tp,
    lat,
    ctx,
    cond_l,
    cond_c,
    shift_w,
    scale_w,
    gate_w,
    lane_table,
    lam,
    gain,
    wq_hbm,
    wk_hbm,
    wv_hbm,
    wo_hbm,
    out,
    wq,
    wk,
    wv,
    wo,
    mod_part,
    mod_recv,
    mod_all,
    raw,
    hidden,
    cos_t,
    sin_t,
    q_send,
    kv_send,
    kvc_send,
    q_buf,
    kv_buf,
    scores,
    o_send,
    heads,
    pair_send,
    pair_recv,
    fin_send,
    fin_recv,
    own_sum,
    w_sem,
    loc_sem,
    mod1_s,
    mod1_r,
    mod2_s,
    mod2_r,
    raw_s,
    raw_r,
    fwd_s,
    fwd_r,
    q_s,
    q_r,
    kv_s,
    kv_r,
    kvc_s,
    kvc_r,
    rel_s,
    rel_r,
    relc_s,
    relc_r,
    o_s,
    o_r,
    pair_s,
    pair_r,
    fin_s,
    fin_r,
):
    own, width = lat.shape
    ctx_rows = ctx.shape[0]
    tok = own * n_tp
    mod_cols = shift_w.shape[1]
    groups = q_send.shape[0]
    ranks = n_sp // groups
    chips = n_tp // 2
    sp_i = lax.axis_index("sp")
    tp_i = lax.axis_index("tp")
    g_i = sp_i // ranks
    r_i = sp_i % ranks
    chip_i = tp_i // 2
    core_i = tp_i % 2
    partner = chip_i * 2 + (1 - core_i)
    pending = []

    def send(src, dst, s_sem, r_sem, **where):
        copy = pltpu.make_async_remote_copy(
            src_ref=src, dst_ref=dst, send_sem=s_sem, recv_sem=r_sem,
            device_id=where, device_id_type=MESH,
        )
        copy.start()
        pending.append(copy)

    def arrived(ref, s_sem, r_sem, **where):
        pltpu.make_async_remote_copy(
            src_ref=ref, dst_ref=ref, send_sem=s_sem, recv_sem=r_sem,
            device_id=where, device_id_type=MESH,
        ).wait_recv()

    loads = [
        pltpu.make_async_copy(src, dst, w_sem.at[i])
        for i, (src, dst) in enumerate(
            ((wk_hbm, wk), (wv_hbm, wv), (wq_hbm, wq), (wo_hbm, wo))
        )
    ]
    for load in loads:
        load.start()

    barrier = pltpu.get_barrier_semaphore()
    for k in range(1, n_sp):
        pl.semaphore_signal(
            barrier, inc=1, device_id={"sp": (sp_i + k) % n_sp}, device_id_type=MESH
        )
    for k in range(1, n_tp):
        pl.semaphore_signal(
            barrier, inc=1, device_id={"tp": (tp_i + k) % n_tp}, device_id_type=MESH
        )

    def silu(v):
        return (v / (1.0 + jnp.exp(-v))).astype(bf16).astype(f32)

    c0 = silu(cond_l[sp_i])
    c1 = silu(cond_c[sp_i])
    row = lax.broadcasted_iota(jnp.int32, (8, c0.shape[-1]), 0)

    def placed_rows(at0, at1):
        zero = jnp.zeros(row.shape, f32)
        rows = jnp.where(row == at0, jnp.broadcast_to(c0, row.shape), zero)
        if at1 is not None:
            rows = jnp.where(row == at1, jnp.broadcast_to(c1, row.shape), rows)
        return rows.astype(bf16)

    mod_part[...] = (
        jnp.dot(placed_rows(0, 1), shift_w[...], preferred_element_type=f32)
        + jnp.dot(placed_rows(2, 3), scale_w[...], preferred_element_type=f32)
        + jnp.dot(placed_rows(4, None), gate_w[...], preferred_element_type=f32)
    )
    pl.semaphore_wait(barrier, n_sp + n_tp - 2)

    for k in range(1, n_sp):
        send(
            mod_part, mod_recv.at[sp_i], mod1_s.at[k], mod1_r.at[sp_i], sp=(sp_i + k) % n_sp
        )
    pieces = raw_s.shape[1]
    piece_rows = own // pieces

    def raw_piece(slot, i):
        return raw.at[slot, pl.ds(i * piece_rows, piece_rows)]

    def send_raw(i):
        for k in range(1, chips):
            send(
                lat.at[pl.ds(i * piece_rows, piece_rows)], raw_piece(tp_i, i),
                raw_s.at[k, i], raw_r.at[chip_i, i],
                tp=((chip_i + k) % chips) * 2 + core_i,
            )

    def relay_raw(i):
        for k in range(1, chips):
            src_chip = (chip_i + chips - k) % chips
            slot = src_chip * 2 + core_i
            arrived(raw_piece(slot, i), raw_s.at[k, i], raw_r.at[src_chip, i], tp=slot)
            send(
                raw_piece(slot, i), raw_piece(slot, i), fwd_s.at[k, i], fwd_r.at[src_chip, i],
                tp=partner,
            )

    early = max(pieces - 1, 1)
    for i in range(early):
        send_raw(i)
    send(lat, raw.at[tp_i], fwd_s.at[0, 0], fwd_r.at[chip_i, 0], tp=partner)
    raw[tp_i] = lat[...]
    mod_recv[sp_i] = mod_part[...]

    tok_row = lax.broadcasted_iota(jnp.int32, (tok, LANES), 0) + sp_i * tok
    grid_row = (tok_row // GRID_W).astype(f32)
    grid_col = (tok_row % GRID_W).astype(f32)
    angles = grid_row * lane_table[0:1, :] + grid_col * lane_table[1:2, :]
    cos_t[...] = jnp.cos(angles)
    sin_t[...] = jnp.sin(angles) * lane_table[2:3, :]

    for k in range(1, n_sp):
        src = (sp_i + n_sp - k) % n_sp
        arrived(mod_recv.at[src], mod1_s.at[k], mod1_r.at[src], sp=src)
    total = mod_recv[0]
    for s in range(1, n_sp):
        total = total + mod_recv[s]
    mod_part2 = mod_all.at[tp_i]
    mod_part2[...] = total
    for k in range(1, n_tp):
        send(
            mod_part2, mod_all.at[tp_i], mod2_s.at[k], mod2_r.at[tp_i], tp=(tp_i + k) % n_tp
        )
    for i in range(early, pieces):
        send_raw(i)
    for i in range(early):
        relay_raw(i)
    for k in range(1, n_tp):
        src = (tp_i + n_tp - k) % n_tp
        arrived(mod_all.at[src], mod2_s.at[k], mod2_r.at[src], tp=src)

    def modulate(x, which, start):
        at = pl.ds(start if isinstance(start, int) else pl.multiple_of(start, 16), x.shape[0])
        factor = lax.rsqrt(jnp.mean(x * x, axis=-1, keepdims=True) + norm_eps)
        for t in range(n_tp):
            cols = slice(t * mod_cols, (t + 1) * mod_cols)
            shift = mod_all[t, which : which + 1, :]
            scale = mod_all[t, which + 2 : which + 3, :]
            hidden[at, cols] = (
                (x[:, cols] * factor) * (1.0 + scale) + shift
            ).astype(bf16)

    half = 2 * own
    lane = lax.broadcasted_iota(jnp.int32, (half, LANES), 1)
    first_quarter = lane % HEAD_DIM < HEAD_DIM // 2
    low_half = lane < HEAD_DIM
    ctx_half = lax.broadcasted_iota(jnp.int32, (ctx_rows, LANES), 1) < HEAD_DIM

    def rope(u, rows):
        swapped = jnp.where(
            first_quarter,
            pltpu.roll(u, LANES - HEAD_DIM // 2, 1),
            pltpu.roll(u, HEAD_DIM // 2, 1),
        )
        return u * cos_t[rows, :] + swapped * sin_t[rows, :]

    def pair_up(a, b, low):
        return (
            jnp.where(low, a, pltpu.roll(b, HEAD_DIM, 1)).astype(bf16),
            jnp.where(low, pltpu.roll(a, HEAD_DIM, 1), b).astype(bf16),
        )

    def lat_slot(s, chip=None):
        if chip is None:
            return kv_buf.at[pl.ds(pl.multiple_of(s * tok, 16), tok)]
        return kv_buf.at[pl.ds(pl.multiple_of(s * tok + chip * half, 16), half)]

    def ctx_slot(s):
        return kv_buf.at[pl.ds(pl.multiple_of(n_sp * tok + s * ctx_rows, 16), ctx_rows)]

    order = list(range(1, groups))
    for c in range(chips):
        chip = (chip_i + c) % chips
        rows = pl.ds(pl.multiple_of(chip * half, 16), half)
        if c == 0:
            modulate(ctx[...].astype(f32), 1, half)
            modulate(raw[tp_i].astype(f32), 0, core_i * own)
            arrived(raw.at[partner], fwd_s.at[0, 0], fwd_r.at[chip_i, 0], tp=partner)
            modulate(raw[partner].astype(f32), 0, (1 - core_i) * own)
            for i in range(early, pieces):
                relay_raw(i)
            count = half + ctx_rows
        else:
            slot = chip * 2 + core_i
            modulate(raw[slot].astype(f32), 0, core_i * own)
            slot = chip * 2 + (1 - core_i)
            for i in range(pieces):
                arrived(
                    raw_piece(slot, i), fwd_s.at[chips - c, i], fwd_r.at[chip, i], tp=partner
                )
            modulate(raw[slot].astype(f32), 0, (1 - core_i) * own)
            count = half
        if c == 0:
            loads[0].wait()
        keys = [jnp.dot(hidden[:count, :], wk[m], preferred_element_type=f32) for m in (0, 1)]
        for p in range(groups // 2):
            slab = slice(p * LANES, (p + 1) * LANES)
            a, b = pair_up(
                rope(keys[0][:half, slab], rows), rope(keys[1][:half, slab], rows), low_half
            )
            kv_send[2 * p, rows, :LANES] = a
            kv_send[2 * p + 1, rows, :LANES] = b
            if c == 0:
                a, b = pair_up(keys[0][half:, slab], keys[1][half:, slab], ctx_half)
                kvc_send[2 * p, :, :LANES] = a
                kvc_send[2 * p + 1, :, :LANES] = b
        if c == 0:
            loads[1].wait()
        vals = jnp.dot(hidden[:count, :], wv[...], preferred_element_type=f32).astype(bf16)
        for j in range(groups):
            slab = slice(j * LANES, (j + 1) * LANES)
            kv_send[j, rows, LANES:] = vals[:half, slab]
            if c == 0:
                kvc_send[j, :, LANES:] = vals[half:, slab]
        for k in order:
            g = (g_i + k) % groups
            to = g * ranks + r_i
            send(
                kv_send.at[g, rows], lat_slot(sp_i, chip), kv_s.at[k, c], kv_r.at[g_i, c], sp=to
            )
            if c == 0:
                send(kvc_send.at[g], ctx_slot(sp_i), kvc_s.at[k], kvc_r.at[g_i], sp=to)
        for e in range(1, ranks):
            to = g_i * ranks + (r_i + e) % ranks
            send(
                kv_send.at[g_i, rows], lat_slot(sp_i, chip), rel_s.at[0, c, e],
                rel_r.at[g_i, c, r_i], sp=to,
            )
            if c == 0:
                send(
                    kvc_send.at[g_i], ctx_slot(sp_i), relc_s.at[0, e], relc_r.at[g_i, r_i], sp=to
                )
        if c == 0:
            loads[2].wait()
        queries = [
            jnp.dot(hidden[:half, :], wq[m], preferred_element_type=f32) for m in (0, 1)
        ]
        for p in range(groups // 2):
            slab = slice(p * LANES, (p + 1) * LANES)
            a, b = pair_up(
                rope(queries[0][:, slab], rows), rope(queries[1][:, slab], rows), low_half
            )
            q_send[2 * p, rows, :] = a
            q_send[2 * p + 1, rows, :] = b
    for k in order:
        g = (g_i + k) % groups
        send(q_send.at[g], q_buf.at[g_i], q_s.at[k], q_r.at[g_i], sp=g * ranks + r_i)
    local = [
        pltpu.make_async_copy(kv_send.at[g_i], lat_slot(sp_i), loc_sem.at[0]),
        pltpu.make_async_copy(kvc_send.at[g_i], ctx_slot(sp_i), loc_sem.at[1]),
        pltpu.make_async_copy(q_send.at[g_i], q_buf.at[g_i], loc_sem.at[2]),
    ]
    for copy in local:
        copy.start()

    for c in range(chips):
        chip = (chip_i + c) % chips
        for k in order:
            g = (g_i + groups - k) % groups
            s = g * ranks + r_i
            arrived(lat_slot(s, chip), kv_s.at[k, c], kv_r.at[g, c], sp=s)
            for e in range(1, ranks):
                to = g_i * ranks + (r_i + e) % ranks
                send(
                    lat_slot(s, chip), lat_slot(s, chip), rel_s.at[k, c, e],
                    rel_r.at[g, c, r_i], sp=to,
                )
            if c == 0:
                arrived(ctx_slot(s), kvc_s.at[k], kvc_r.at[g], sp=s)
                for e in range(1, ranks):
                    to = g_i * ranks + (r_i + e) % ranks
                    send(
                        ctx_slot(s), ctx_slot(s), relc_s.at[k, e], relc_r.at[g, r_i], sp=to
                    )
    for copy in local:
        copy.wait()
    for e in range(1, ranks):
        r = (r_i + ranks - e) % ranks
        to = g_i * ranks + r
        for k in range(groups):
            g = (g_i + groups - k) % groups
            s = g * ranks + r
            for c in range(chips):
                chip = (chip_i + c) % chips
                arrived(lat_slot(s, chip), rel_s.at[k, c, e], rel_r.at[g, c, r], sp=to)
            arrived(ctx_slot(s), relc_s.at[k, e], relc_r.at[g, r], sp=to)

    key_total = kv_buf.shape[0]
    q_tile = scores.shape[0] // 2
    block = pick(key_total, 512, LANES)
    coef = HEAD_DIM ** (-0.5) * 1.4426950408889634
    q_low = lax.broadcasted_iota(jnp.int32, (q_tile, LANES), 1) < HEAD_DIM
    head_lam = lam[g_i]
    tiles = tok // q_tile
    head_gain = gain[g_i]

    def attend(g, start):
        q = q_buf[g, pl.ds(start, q_tile), :]
        zero = jnp.zeros_like(q)
        q2 = jnp.concatenate([jnp.where(q_low, q, zero), jnp.where(q_low, zero, q)], axis=0)
        peak = None
        for b in range(key_total // block):
            rows = slice(b * block, (b + 1) * block)
            s = lax.dot_general(
                q2, kv_buf[rows, :LANES], (((1,), (1,)), ((), ())), preferred_element_type=f32
            )
            scores[:, rows] = s
            for c in range(block // LANES):
                piece = s[:, c * LANES : (c + 1) * LANES]
                peak = piece if peak is None else jnp.maximum(peak, piece)
        top = jnp.max(peak, axis=-1, keepdims=True) * coef
        sums = None
        acc = None
        for b in range(key_total // block):
            rows = slice(b * block, (b + 1) * block)
            w = jnp.exp2(scores[:, rows] * coef - top)
            for c in range(block // LANES):
                piece = w[:, c * LANES : (c + 1) * LANES]
                sums = piece if sums is None else sums + piece
            part = jnp.dot(w.astype(bf16), kv_buf[rows, LANES:], preferred_element_type=f32)
            acc = part if acc is None else acc + part
        mean_v = acc / jnp.sum(sums, axis=-1, keepdims=True)
        mixed = mean_v[:q_tile] - head_lam * mean_v[q_tile:]
        factor = lax.rsqrt(jnp.mean(mixed * mixed, axis=-1, keepdims=True) + norm_eps)
        o_send[g, pl.ds(start, q_tile), :] = (mixed * factor * head_gain).astype(bf16)

    def o_copy(k, i):
        g = (g_i + groups - k) % groups
        rows = pl.ds(pl.multiple_of(i * q_tile, 16), q_tile)
        return pltpu.make_async_remote_copy(
            src_ref=o_send.at[g, rows], dst_ref=heads.at[g_i, rows], send_sem=o_s.at[k, i],
            recv_sem=o_r.at[g_i, i], device_id={"sp": g * ranks + r_i}, device_id_type=MESH,
        )

    @pl.loop(0, groups)
    def _(k):
        g = (g_i + groups - k) % groups

        @pl.when(k > 0)
        def _():
            arrived(q_buf.at[g], q_s.at[k], q_r.at[g], sp=g * ranks + r_i)

        @pl.loop(0, tiles)
        def _(i):
            attend(g, pl.multiple_of(i * q_tile, q_tile))

            @pl.when(k > 0)
            def _():
                o_copy(k, i).start()

    heads[g_i] = o_send[g_i]
    loads[3].wait()
    for k in order:
        src = (g_i + k) % groups
        for i in range(tiles):
            rows = pl.ds(i * q_tile, q_tile)
            arrived(heads.at[src, rows], o_s.at[k, i], o_r.at[src, i], sp=src * ranks + r_i)

    parts = pair_send.shape[1]
    part_cols = width // parts

    def head_rows(chunk):
        start = pl.multiple_of(chunk * own, 16)
        return jnp.concatenate(
            [heads[h, pl.ds(start, own), :] for h in range(groups)], axis=-1
        )

    def term(left, p):
        cols = slice(p * part_cols, (p + 1) * part_cols)
        return jnp.dot(left, wo[:, cols], preferred_element_type=f32).astype(bf16)

    def to_partner(k):
        chip = (chip_i + 1 + k) % chips
        left = head_rows(chip * 2 + (1 - core_i))
        for p in range(parts):
            pair_send[k, p] = term(left, p)
            send(
                pair_send.at[k, p], pair_recv.at[k, p], pair_s.at[k, p], pair_r.at[k, p],
                tp=partner,
            )

    def with_partner(k):
        chip = (chip_i + 1 + k) % chips
        left = head_rows(chip * 2 + core_i)
        for p in range(parts):
            mine = term(left, p).astype(f32)
            arrived(pair_recv.at[k, p], pair_s.at[k, p], pair_r.at[k, p], tp=partner)
            both = mine + pair_recv[k, p].astype(f32)
            if k < chips - 1:
                fin_send[k, p] = both.astype(bf16)
                send(
                    fin_send.at[k, p], fin_recv.at[k, p], fin_s.at[k, p], fin_r.at[k, p],
                    tp=chip * 2 + core_i,
                )
            else:
                own_sum[p] = both

    for k in range(chips - 1):
        to_partner(k)
    for k in range(chips - 1):
        with_partner(k)
    to_partner(chips - 1)
    with_partner(chips - 1)
    for p in range(parts):
        summed = own_sum[p]
        for k in range(chips - 1):
            src_chip = (chip_i + chips - 1 - k) % chips
            arrived(
                fin_recv.at[k, p], fin_s.at[k, p], fin_r.at[k, p], tp=src_chip * 2 + core_i
            )
            summed = summed + fin_recv[k, p].astype(f32)
        cols = slice(p * part_cols, (p + 1) * part_cols)
        per = mod_cols // part_cols
        if per >= 1:
            low = (p % per) * part_cols
            gate = mod_all[p // per, 4:5, low : low + part_cols]
        else:
            span = part_cols // mod_cols
            gate = jnp.concatenate(
                [mod_all[p * span + q, 4:5, :] for q in range(span)], axis=-1
            )
        out[:, cols] = (lat[:, cols].astype(f32) + gate * summed).astype(bf16)
    for copy in pending:
        copy.wait_send()
    for k in order:
        for i in range(tiles):
            o_copy(k, i).wait_send()


def local(
    n_sp,
    n_tp,
    latent,
    context,
    cond_latent,
    cond_context,
    shift_weight,
    scale_weight,
    gate_weight,
    query_weight,
    key_weight,
    value_weight,
    out_weight,
    lambda_heads,
    out_gain,
):
    own, width = latent.shape
    ctx_rows = context.shape[0]
    tok = own * n_tp
    groups = lambda_heads.shape[0]
    ranks = n_sp // groups
    chips = n_tp // 2
    mod_rows, mod_cols = shift_weight.shape
    keys = n_sp * (tok + ctx_rows)
    q_tile = pick(tok, 128, 16)
    pieces = 3 if own % 48 == 0 else 1
    parts = 4 if width % (4 * LANES) == 0 else 1

    quarter = HEAD_DIM // 4
    inverse = np.float32(rope_theta) ** (-np.arange(quarter, dtype=np.float32) / quarter)
    zeros = np.zeros((quarter,), np.float32)
    repeat = LANES // (2 * quarter)
    half = np.ones((2 * quarter,), np.float32)
    lane_table = np.zeros((8, LANES), np.float32)
    lane_table[0] = np.tile(np.concatenate([inverse, zeros]), repeat)
    lane_table[1] = np.tile(np.concatenate([zeros, inverse]), repeat)
    lane_table[2] = np.tile(np.concatenate([-half, half]), repeat // 2)
    gain = out_gain.reshape(groups, 1, VALUE_DIM)
    vmem = pl.BlockSpec(memory_space=pltpu.VMEM)
    hbm = pl.BlockSpec(memory_space=pl.ANY)
    dma = pltpu.SemaphoreType.DMA
    scratch = [
        pltpu.VMEM(query_weight.shape, bf16),
        pltpu.VMEM(key_weight.shape, bf16),
        pltpu.VMEM(value_weight.shape, bf16),
        pltpu.VMEM(out_weight.shape, bf16),
        pltpu.VMEM((8, mod_cols), f32),
        pltpu.VMEM((n_sp, 8, mod_cols), f32),
        pltpu.VMEM((n_tp, 8, mod_cols), f32),
        pltpu.VMEM((n_tp, own, width), bf16),
        pltpu.VMEM((2 * own + ctx_rows, width), bf16),
        pltpu.VMEM((tok, LANES), f32),
        pltpu.VMEM((tok, LANES), f32),
        pltpu.VMEM((groups, tok, LANES), bf16),
        pltpu.VMEM((groups, tok, 2 * LANES), bf16),
        pltpu.VMEM((groups, ctx_rows, 2 * LANES), bf16),
        pltpu.VMEM((groups, tok, LANES), bf16),
        pltpu.VMEM((keys, 2 * LANES), bf16),
        pltpu.VMEM((2 * q_tile, keys), f32),
        pltpu.VMEM((groups, tok, LANES), bf16),
        pltpu.VMEM((groups, tok, LANES), bf16),
        pltpu.VMEM((chips, parts, own, width // parts), bf16),
        pltpu.VMEM((chips, parts, own, width // parts), bf16),
        pltpu.VMEM((max(chips - 1, 1), parts, own, width // parts), bf16),
        pltpu.VMEM((max(chips - 1, 1), parts, own, width // parts), bf16),
        pltpu.VMEM((parts, own, width // parts), f32),
        dma((4,)),
        dma((3,)),
        dma((n_sp,)),
        dma((n_sp,)),
        dma((n_tp,)),
        dma((n_tp,)),
        dma((chips, pieces)),
        dma((chips, pieces)),
        dma((chips, pieces)),
        dma((chips, pieces)),
        dma((groups,)),
        dma((groups,)),
        dma((groups, chips)),
        dma((groups, chips)),
        dma((groups,)),
        dma((groups,)),
        dma((groups, chips, ranks)),
        dma((groups, chips, ranks)),
        dma((groups, ranks)),
        dma((groups, ranks)),
        dma((groups, tok // q_tile)),
        dma((groups, tok // q_tile)),
        dma((chips, parts)),
        dma((chips, parts)),
        dma((chips, parts)),
        dma((chips, parts)),
    ]
    return pl.pallas_call(
        functools.partial(body, n_sp, n_tp),
        out_shape=jax.ShapeDtypeStruct((own, width), bf16),
        in_specs=[vmem] * 8 + [pl.BlockSpec(memory_space=pltpu.SMEM), vmem] + [hbm] * 4,
        out_specs=vmem,
        scratch_shapes=scratch,
        compiler_params=pltpu.CompilerParams(
            collective_id=0, has_side_effects=True, vmem_limit_bytes=60 * 1024 * 1024
        ),
        name="diff_attention",
    )(
        latent,
        context,
        cond_latent.reshape(n_sp, 1, mod_rows),
        cond_context.reshape(n_sp, 1, mod_rows),
        shift_weight,
        scale_weight,
        gate_weight,
        jnp.asarray(lane_table),
        lambda_heads,
        gain,
        query_weight,
        key_weight,
        value_weight,
        out_weight,
    )


def solution(mesh):
    placed = (
        P(("sp", "tp"), None),
        P("sp", None),
        P(),
        P(),
        P("sp", "tp"),
        P("sp", "tp"),
        P("sp", "tp"),
        P(None, None, "tp"),
        P(None, None, "tp"),
        P(None, "tp"),
        P("tp", None),
        P("tp"),
        P("tp"),
    )
    return jax.shard_map(
        functools.partial(local, mesh.shape["sp"], mesh.shape["tp"]),
        mesh=mesh,
        in_specs=placed,
        out_specs=P(("sp", "tp"), None),
        check_vma=False,
    )
```
